32 devices in a mesh: fs: 8 (over z, y), tp: 4 (over x, core).
Axes of the slice: x: 2, y: 2, z: 4, core: 2. Of those that a mesh axis runs over, the one named last changes fastest.
Arguments:
- saved_input: bfloat16 [16384, 2048], P('fs'), may hold values from -6 to 6
- query_cotangent: bfloat16 [16384, 2048], P('fs', 'tp'), may hold values from -0.046875 to 0.046875
- forget_cotangent: bfloat16 [16384, 2048], P('fs', 'tp'), may hold values from -0.046875 to 0.046875
- mixed_output: bfloat16 [16384, 2048], P('fs', 'tp'), may hold values from -6 to 6
- out_cotangent: bfloat16 [16384, 2048], P('fs'), may hold values from -0.046875 to 0.046875
- query_basis: bfloat16 [2048, 256], replicated, may hold values from -0.125 to 0.125
- forget_basis: bfloat16 [2048, 256], replicated, may hold values from -0.125 to 0.125
- out_basis: bfloat16 [2048, 256], replicated, may hold values from -0.125 to 0.125
- query_weight: float32 [2048, 2048], P('fs', 'tp'), may hold values from -0.125 to 0.125
- forget_weight: float32 [2048, 2048], P('fs', 'tp'), may hold values from -0.125 to 0.125
- out_weight: float32 [2048, 2048], P('fs', 'tp'), may hold values from -0.125 to 0.125
- query_first: float32 [256, 2048], P('fs', 'tp'), may hold values from -25 to 25
- forget_first: float32 [256, 2048], P('fs', 'tp'), may hold values from -25 to 25
- out_first: float32 [256, 2048], P('fs', 'tp'), may hold values from -25 to 25
- query_second: float32 [256, 2048], P('fs', 'tp'), may hold values from 0.2 to 2
- forget_second: float32 [256, 2048], P('fs', 'tp'), may hold values from 0.2 to 2
- out_second: float32 [256, 2048], P('fs', 'tp'), may hold values from 0.2 to 2
Outputs:
- query_update: float32 [2048, 2048], P('fs', 'tp')
- forget_update: float32 [2048, 2048], P('fs', 'tp')
- out_update: float32 [2048, 2048], P('fs', 'tp')
- query_first_new: float32 [256, 2048], P('fs', 'tp')
- forget_first_new: float32 [256, 2048], P('fs', 'tp')
- out_first_new: float32 [256, 2048], P('fs', 'tp')
- query_second_new: float32 [256, 2048], P('fs', 'tp')
- forget_second_new: float32 [256, 2048], P('fs', 'tp')
- out_second_new: float32 [256, 2048], P('fs', 'tp')
- query_copy: bfloat16 [2048, 2048], P(None, 'tp')
- forget_copy: bfloat16 [2048, 2048], P(None, 'tp')
- out_copy: bfloat16 [2048, 2048], P(None, 'tp')
The draws below stay inside these ranges and needn't reach their ends.
All inputs are finite; a program needn't handle non-finite values.
Results may differ from the reference program's by a relative error of at most 0.0065.
Values may be sent and summed in bfloat16 or wider, within the bound.
A program may use at most 128 MiB of HBM per device.

```python
import math
import jax
import jax.numpy as jnp
from jax import lax

D = 2048
WIDTH = 2048
RANK = 256
TOKENS = 16384


def moment_draw(key):
    key_rows = jax.random.fold_in(key, 11)
    key_cols = jax.random.fold_in(key, 12)
    key_base = jax.random.fold_in(key, 13)
    ramp_rows = jnp.arange(RANK, dtype=jnp.float32) / RANK
    ramp_cols = jnp.arange(WIDTH, dtype=jnp.float32) / WIDTH
    row_scale = jnp.exp(jnp.log(3.0) * (ramp_rows + jax.random.uniform(key_rows, (RANK,), jnp.float32)))
    col_scale = jnp.exp(jnp.log(3.0) * (ramp_cols + jax.random.uniform(key_cols, (WIDTH,), jnp.float32)))
    base = jnp.clip(jax.random.normal(key_base, (RANK, WIDTH), jnp.float32), -4.0, 4.0)
    return 0.075 * base * row_scale[:, None] * col_scale[None, :]


def draw_query_first(key, part):
    return moment_draw(jax.random.fold_in(key, 101))


def draw_forget_first(key, part):
    return moment_draw(jax.random.fold_in(key, 202))


def draw_out_first(key, part):
    return moment_draw(jax.random.fold_in(key, 303))


def block_scale(key, dims, split, low, high):
    level, own = 1.0, jax.random.fold_in(key, 6)
    for position, blocks in split:
        draws = jnp.exp(jax.random.uniform(jax.random.fold_in(own, position), (blocks,), jnp.float32, low / len(split), high / len(split)))
        level = level * jnp.repeat(draws, dims[position] // blocks).reshape([-1 if axis == position else 1 for axis in range(len(dims))])
    return level


def scatter_about(key, extent, scale, most, cuts=(), held_as=jnp.bfloat16):
    entries = jax.random.normal(key, extent, jnp.float32) * scale
    if len(cuts) > 0:
        entries = block_scale(key, extent, cuts, -0.22, 0.18) * entries
    return jnp.clip(entries, min=-most, max=most).astype(held_as)


def setup_inputs(seed: int = 0) -> dict:
    arg_keys = jax.random.split(jax.random.key(seed), 18)
    saved_input = scatter_about(arg_keys[0], (TOKENS, D), 1.0, 6.0, ((0, 8),))
    query_cotangent = scatter_about(arg_keys[1], (TOKENS, WIDTH), (TOKENS ** -0.5), 0.046875, ((0, 8), (1, 4)))
    forget_cotangent = scatter_about(arg_keys[2], (TOKENS, WIDTH), (TOKENS ** -0.5), 0.046875, ((0, 8), (1, 4)))
    mixed_output = scatter_about(arg_keys[3], (TOKENS, WIDTH), 1.0, 6.0, ((0, 8), (1, 4)))
    out_cotangent = scatter_about(arg_keys[4], (TOKENS, D), (TOKENS ** -0.5), 0.046875, ((0, 8),))
    query_basis = scatter_about(arg_keys[5], (D, RANK), D ** -0.5, 0.125)
    forget_basis = scatter_about(arg_keys[6], (D, RANK), D ** -0.5, 0.125)
    out_basis = scatter_about(arg_keys[7], (D, RANK), D ** -0.5, 0.125)
    query_weight = scatter_about(arg_keys[8], (D, WIDTH), D ** -0.5, 0.125, ((0, 8), (1, 4)), jnp.float32)
    forget_weight = scatter_about(arg_keys[9], (D, WIDTH), D ** -0.5, 0.125, ((0, 8), (1, 4)), jnp.float32)
    out_weight = scatter_about(arg_keys[10], (D, WIDTH), WIDTH ** -0.5, 0.125, ((0, 8), (1, 4)), jnp.float32)
    query_first = draw_query_first(jax.random.fold_in(arg_keys[17], 71), 0)
    forget_first = draw_forget_first(jax.random.fold_in(arg_keys[17], 71), 0)
    out_first = draw_out_first(jax.random.fold_in(arg_keys[17], 71), 0)
    query_second = jnp.clip(jnp.exp(math.log(2.0) - 2.3025851 * jax.random.uniform(arg_keys[14], (RANK, WIDTH), jnp.float32) ** block_scale(arg_keys[14], (RANK, WIDTH), ((0, 8), (1, 4)), -0.2, 0.2)), 0.2, 2.0)
    forget_second = jnp.clip(jnp.exp(math.log(2.0) - 2.3025851 * jax.random.uniform(arg_keys[15], (RANK, WIDTH), jnp.float32) ** block_scale(arg_keys[15], (RANK, WIDTH), ((0, 8), (1, 4)), -0.2, 0.2)), 0.2, 2.0)
    out_second = jnp.clip(jnp.exp(math.log(2.0) - 2.3025851 * jax.random.uniform(arg_keys[16], (RANK, WIDTH), jnp.float32) ** block_scale(arg_keys[16], (RANK, WIDTH), ((0, 8), (1, 4)), -0.2, 0.2)), 0.2, 2.0)
    return {"saved_input": saved_input, "query_cotangent": query_cotangent, "forget_cotangent": forget_cotangent, "mixed_output": mixed_output, "out_cotangent": out_cotangent, "query_basis": query_basis, "forget_basis": forget_basis, "out_basis": out_basis, "query_weight": query_weight, "forget_weight": forget_weight, "out_weight": out_weight, "query_first": query_first, "forget_first": forget_first, "out_first": out_first, "query_second": query_second, "forget_second": forget_second, "out_second": out_second}


def one_matrix(source, cotangent, basis, weight, first, second):
    gradient = jnp.dot(source.T, cotangent, preferred_element_type=jnp.float32)
    basis_wide = basis.astype(jnp.float32)
    projected = jnp.dot(basis_wide.T, gradient, precision=lax.Precision.HIGHEST)
    first_new = 0.8 * first + 0.2 * projected
    second_new = 0.95 * second + 0.05 * projected * projected
    direction = first_new / (jnp.sqrt(second_new) + 1e-08)
    scale = lax.rsqrt(jnp.sum(direction * direction) / (RANK * WIDTH) + 1e-06)
    update = jnp.dot(basis_wide, direction, precision=lax.Precision.HIGHEST) * scale
    copy = (weight - 0.05 * update).astype(jnp.bfloat16)
    return (update, first_new, second_new, copy)

def reference(saved_input, query_cotangent, forget_cotangent, mixed_output, out_cotangent, query_basis, forget_basis, out_basis, query_weight, forget_weight, out_weight, query_first, forget_first, out_first, query_second, forget_second, out_second):
    q_update, q_first, q_second, q_copy = one_matrix(saved_input, query_cotangent, query_basis, query_weight, query_first, query_second)
    f_update, f_first, f_second, f_copy = one_matrix(saved_input, forget_cotangent, forget_basis, forget_weight, forget_first, forget_second)
    o_update, o_first, o_second, o_copy = one_matrix(out_cotangent, mixed_output, out_basis, out_weight, out_first, out_second)
    return (q_update, f_update, o_update, q_first, f_first, o_first, q_second, f_second, o_second, q_copy, f_copy, o_copy)
```

```python
import functools

import jax
import jax.numpy as jnp
from jax import lax
from jax.experimental import pallas as pl
from jax.experimental.pallas import tpu as pltpu
from jax.sharding import PartitionSpec as P

MESH = pl.DeviceIdType.MESH
ANY = pl.ANY
VMEM = pltpu.VMEM


def kernel(
    n,
    tp_n,
    chunk,
    saved_hbm,
    outcot_hbm,
    qcot_hbm,
    fcot_hbm,
    mixed_hbm,
    qb_hbm,
    fb_hbm,
    ob_hbm,
    qw,
    fw,
    ow,
    q1,
    f1,
    o1,
    q2,
    f2,
    o2,
    qup,
    fup,
    oup,
    q1n,
    f1n,
    o1n,
    q2n,
    f2n,
    o2n,
    qc,
    fc,
    oc,
    src,
    cot,
    bas,
    acc,
    part,
    rs_buf,
    dirs,
    gath,
    stage,
    sq_own,
    sq_buf,
    src_sem,
    cot_sem,
    bas_sem,
    rs_send,
    rs_recv,
    ag_send,
    ag_recv,
    w_send,
    w_recv,
    sq_send,
    sq_recv,
    out_sem,
):
    me = lax.axis_index("fs")
    tp = lax.axis_index("tp")
    weights, firsts, seconds = (qw, fw, ow), (q1, f1, o1), (q2, f2, o2)
    updates, firsts_new, seconds_new = (qup, fup, oup), (q1n, f1n, o1n), (q2n, f2n, o2n)
    copies = (qc, fc, oc)
    tokens = saved_hbm.shape[0]
    rank, cols = acc.shape
    rows = qw.shape[0]
    rp = rank // n
    n_chunks = tokens // chunk
    half = n // 2
    y = lax.rem(me, 2)
    o = me // 2
    partner = o * 2 + 1 - y

    def src_copy(s, c):
        return pltpu.make_async_copy(
            (saved_hbm, outcot_hbm)[s].at[pl.ds(c * chunk, chunk)],
            src.at[s, pl.ds(c * chunk, chunk)],
            src_sem.at[s, c],
        )

    def cot_copy(m):
        return pltpu.make_async_copy((qcot_hbm, fcot_hbm, mixed_hbm)[m], cot.at[m], cot_sem.at[m])

    def bas_copy(m):
        return pltpu.make_async_copy((qb_hbm, fb_hbm, ob_hbm)[m], bas.at[m], bas_sem.at[m])

    bas_copy(0).start()
    src_copy(0, 0).start()
    cot_copy(0).start()
    for c in range(1, n_chunks):
        src_copy(0, c).start()
    bas_copy(1).start()
    cot_copy(1).start()
    bas_copy(2).start()
    for c in range(n_chunks):
        src_copy(1, c).start()
    cot_copy(2).start()

    for m in range(3):
        gath[m, me] = weights[m][...].astype(jnp.bfloat16)

    barrier = pltpu.get_barrier_semaphore()
    for k in range(1, n):
        pl.semaphore_signal(
            barrier, inc=1, device_id={"fs": lax.rem(me + k, n)}, device_id_type=MESH
        )
    for k in range(1, tp_n):
        pl.semaphore_signal(
            barrier, inc=1, device_id={"tp": lax.rem(tp + k, tp_n)}, device_id_type=MESH
        )
    pl.semaphore_wait(barrier, n - 1 + tp_n - 1)

    def w_copy(m, block, target, send_sem):
        return pltpu.make_async_remote_copy(
            src_ref=gath.at[m, block],
            dst_ref=gath.at[m, block],
            send_sem=send_sem,
            recv_sem=w_recv.at[m, block],
            device_id={"fs": target},
            device_id_type=MESH,
        )

    def w_wait(block):
        for m in range(3):
            w_copy(m, block, partner, w_send.at[0, m, 0]).wait_recv()

    def w_round(r, act):
        below, above = o - r, o + r
        if r < half - 1:

            @pl.when(jnp.logical_and(below >= 0, o + 1 < half))
            def _():
                for m in range(3):
                    act(w_copy(m, below * 2 + y, me + 2, w_send.at[0, m, r]))

            @pl.when(jnp.logical_and(above < half, o >= 1))
            def _():
                for m in range(3):
                    act(w_copy(m, above * 2 + y, me - 2, w_send.at[1, m, r]))

        @pl.when(below >= 0)
        def _():
            for m in range(3):
                act(w_copy(m, below * 2 + y, partner, w_send.at[2, m, r]))

        if r > 0:

            @pl.when(above < half)
            def _():
                for m in range(3):
                    act(w_copy(m, above * 2 + y, partner, w_send.at[3, m, r]))

    def w_start(r):
        if r > 0:

            @pl.when(o - r >= 0)
            def _():
                w_wait((o - r) * 2 + y)

            @pl.when(o + r < half)
            def _():
                w_wait((o + r) * 2 + y)

        w_round(r, lambda copy: copy.start())

    w_start(0)

    def rs_copy(m, k):
        peer = lax.rem(me + k, n)
        return pltpu.make_async_remote_copy(
            src_ref=part.at[m, pl.ds(pl.multiple_of(peer * rp, rp), rp)],
            dst_ref=rs_buf.at[m, k - 1],
            send_sem=rs_send.at[m, k - 1],
            recv_sem=rs_recv.at[m, k - 1],
            device_id={"fs": peer},
            device_id_type=MESH,
        )

    mine = pl.ds(pl.multiple_of(me * rp, rp), rp)

    def ag_copy(m, k):
        peer = lax.rem(me + k, n)
        return pltpu.make_async_remote_copy(
            src_ref=dirs.at[m, mine],
            dst_ref=dirs.at[m, mine],
            send_sem=ag_send.at[m, k - 1],
            recv_sem=ag_recv.at[m, k - 1],
            device_id={"fs": peer},
            device_id_type=MESH,
        )

    def project(m):
        s = (0, 0, 1)[m]
        bas_copy(m).wait()
        cot_copy(m).wait()
        if m != 1:
            for c in range(n_chunks):
                src_copy(s, c).wait()

        acc[...] = jnp.zeros_like(acc)

        def body(c, carry):
            at = pl.ds(pl.multiple_of(c * chunk, chunk), chunk)
            reduced = jnp.dot(
                src[s, at, :], bas[m], preferred_element_type=jnp.float32
            ).astype(jnp.bfloat16)
            acc[...] += lax.dot_general(
                reduced,
                cot[m, at, :],
                (((0,), (0,)), ((), ())),
                preferred_element_type=jnp.float32,
            )
            return carry

        lax.fori_loop(0, n_chunks, body, 0)
        part[m] = acc[...].astype(jnp.bfloat16)
        for k in range(1, n):
            rs_copy(m, k).start()

    project(0)
    project(1)
    w_start(1)
    project(2)

    for m in range(3):
        projected = part[m, mine, :].astype(jnp.float32)
        for k in range(1, n):
            rs_copy(m, k).wait_recv()
            projected += rs_buf[m, k - 1].astype(jnp.float32)
        first_new = 0.8 * firsts[m][...] + 0.2 * projected
        second_new = 0.95 * seconds[m][...] + 0.05 * projected * projected
        firsts_new[m][...] = first_new
        seconds_new[m][...] = second_new
        direction = first_new / (jnp.sqrt(second_new) + 1e-08)
        dirs[m, mine, :] = direction.astype(jnp.bfloat16)
        for k in range(1, n):
            ag_copy(m, k).start()

    for r in range(2, half):
        w_start(r)

    sums = []
    for m in range(3):
        for k in range(1, n):
            peer = lax.rem(me + n - k, n)
            pltpu.make_async_remote_copy(
                src_ref=dirs.at[m, mine],
                dst_ref=dirs.at[m, pl.ds(pl.multiple_of(peer * rp, rp), rp)],
                send_sem=ag_send.at[m, k - 1],
                recv_sem=ag_recv.at[m, k - 1],
                device_id={"fs": peer},
                device_id_type=MESH,
            ).wait_recv()
        wide = dirs[m].astype(jnp.float32)
        sums.append(jnp.sum(wide * wide))
    line = lax.broadcasted_iota(jnp.int32, sq_own.shape, 0)
    sq_own[...] = jnp.where(line == 0, sums[0], jnp.where(line == 1, sums[1], sums[2]))

    def sq_copy(k):
        return pltpu.make_async_remote_copy(
            src_ref=sq_own,
            dst_ref=sq_buf.at[k - 1],
            send_sem=sq_send.at[k - 1],
            recv_sem=sq_recv.at[k - 1],
            device_id={"tp": lax.rem(tp + k, tp_n)},
            device_id_type=MESH,
        )

    for k in range(1, tp_n):
        sq_copy(k).start()
    total = sq_own[...]
    for k in range(1, tp_n):
        sq_copy(k).wait_recv()
        total += sq_buf[k - 1]
    scale = lax.rsqrt(total / (rank * cols * tp_n) + 1e-06)

    def out_copy(m, block):
        return pltpu.make_async_copy(
            stage.at[m, block],
            copies[m].at[pl.ds(pl.multiple_of(block * rows, rows), rows)],
            out_sem.at[m, block],
        )

    def step_of(m, block):
        at = pl.ds(pl.multiple_of(block * rows, rows), rows)
        return jnp.dot(bas[m, at, :], dirs[m], preferred_element_type=jnp.float32)

    for m in range(3):
        update = step_of(m, me) * scale[m : m + 1, :1]
        updates[m][...] = update
        stage[m, me] = (weights[m][...] - 0.05 * update).astype(jnp.bfloat16)
        out_copy(m, me).start()

    def finish(block):
        for m in range(3):
            stage[m, block] = (
                gath[m, block].astype(jnp.float32)
                - step_of(m, block) * (0.05 * scale[m : m + 1, :1])
            ).astype(jnp.bfloat16)
            out_copy(m, block).start()

    def near(i, carry):
        finish(lax.rem(o + i, half) * 2 + y)
        return carry

    def far(i, carry):
        block = lax.rem(o + i, half) * 2 + 1 - y
        w_wait(block)
        finish(block)
        return carry

    lax.fori_loop(1, half, near, 0)
    lax.fori_loop(0, half, far, 0)

    for r in range(half):
        w_round(r, lambda copy: copy.wait_send())
    for m in range(3):
        for k in range(1, n):
            rs_copy(m, k).wait_send()
            ag_copy(m, k).wait_send()
    for k in range(1, tp_n):
        sq_copy(k).wait_send()

    def drain(block, carry):
        for m in range(3):
            out_copy(m, block).wait()
        return carry

    lax.fori_loop(0, n, drain, 0)


def local(
    n,
    tp_n,
    saved_input,
    query_cotangent,
    forget_cotangent,
    mixed_output,
    out_cotangent,
    query_basis,
    forget_basis,
    out_basis,
    query_weight,
    forget_weight,
    out_weight,
    query_first,
    forget_first,
    out_first,
    query_second,
    forget_second,
    out_second,
):
    tokens, width = saved_input.shape
    rank = query_basis.shape[1]
    rows, cols = query_weight.shape
    rp = rank // n
    half = n // 2
    chunk = min(512, tokens)
    f32, bf16 = jnp.float32, jnp.bfloat16
    dma = pltpu.SemaphoreType.DMA
    shape = jax.ShapeDtypeStruct
    return pl.pallas_call(
        functools.partial(kernel, n, tp_n, chunk),
        out_shape=(shape((rows, cols), f32),) * 3
        + (shape((rp, cols), f32),) * 6
        + (shape((n * rows, cols), bf16),) * 3,
        in_specs=[pl.BlockSpec(memory_space=ANY)] * 8 + [pl.BlockSpec(memory_space=VMEM)] * 9,
        out_specs=(pl.BlockSpec(memory_space=VMEM),) * 9 + (pl.BlockSpec(memory_space=ANY),) * 3,
        scratch_shapes=[
            VMEM((2, tokens, width), bf16),
            VMEM((3, tokens, cols), bf16),
            VMEM((3, width, rank), bf16),
            VMEM((rank, cols), f32),
            VMEM((3, rank, cols), bf16),
            VMEM((3, n - 1, rp, cols), bf16),
            VMEM((3, rank, cols), bf16),
            VMEM((3, n, rows, cols), bf16),
            VMEM((3, n, rows, cols), bf16),
            VMEM((8, 128), f32),
            VMEM((tp_n - 1, 8, 128), f32),
            dma((2, tokens // chunk)),
            dma((3,)),
            dma((3,)),
            dma((3, n - 1)),
            dma((3, n - 1)),
            dma((3, n - 1)),
            dma((3, n - 1)),
            dma((4, 3, half)),
            dma((3, n)),
            dma((tp_n - 1,)),
            dma((tp_n - 1,)),
            dma((3, n)),
        ],
        compiler_params=pltpu.CompilerParams(
            collective_id=0, has_side_effects=True, vmem_limit_bytes=63 * 1024 * 1024
        ),
    )(
        saved_input,
        out_cotangent,
        query_cotangent,
        forget_cotangent,
        mixed_output,
        query_basis,
        forget_basis,
        out_basis,
        query_weight,
        forget_weight,
        out_weight,
        query_first,
        forget_first,
        out_first,
        query_second,
        forget_second,
        out_second,
    )


def solution(mesh):
    split = P("fs", "tp")
    in_specs = (
        (P("fs", None), split, split, split, P("fs", None)) + (P(),) * 3 + (split,) * 9
    )
    out_specs = (split,) * 9 + (P(None, "tp"),) * 3
    return jax.shard_map(
        functools.partial(local, mesh.shape["fs"], mesh.shape["tp"]),
        mesh=mesh,
        in_specs=in_specs,
        out_specs=out_specs,
        check_vma=False,
    )
```

```python
import functools

import jax
import jax.numpy as jnp
from jax import lax
from jax.experimental import pallas as pl
from jax.experimental.pallas import tpu as pltpu
from jax.sharding import PartitionSpec as P

MESH = pl.DeviceIdType.MESH
ANY = pl.ANY
VMEM = pltpu.VMEM


def kernel(
    n,
    tp_n,
    chunk,
    saved_hbm,
    outcot_hbm,
    qcot_hbm,
    fcot_hbm,
    mixed_hbm,
    qb_hbm,
    fb_hbm,
    ob_hbm,
    qw,
    fw,
    ow,
    q1,
    f1,
    o1,
    q2,
    f2,
    o2,
    qup,
    fup,
    oup,
    q1n,
    f1n,
    o1n,
    q2n,
    f2n,
    o2n,
    qc,
    fc,
    oc,
    src,
    cot,
    bas,
    acc,
    part,
    rs_buf,
    dirs,
    gath,
    stage,
    sq_own,
    sq_buf,
    src_sem,
    cot_sem,
    bas_sem,
    rs_send,
    rs_recv,
    ag_send,
    ag_recv,
    w_send,
    w_recv,
    sq_send,
    sq_recv,
    out_sem,
):
    me = lax.axis_index("fs")
    tp = lax.axis_index("tp")
    weights, firsts, seconds = (qw, fw, ow), (q1, f1, o1), (q2, f2, o2)
    updates, firsts_new, seconds_new = (qup, fup, oup), (q1n, f1n, o1n), (q2n, f2n, o2n)
    copies = (qc, fc, oc)
    tokens = saved_hbm.shape[0]
    rank, cols = acc.shape
    rows = qw.shape[0]
    rp = rank // n
    n_chunks = tokens // chunk
    half = n // 2
    y = lax.rem(me, 2)
    o = me // 2
    partner = o * 2 + 1 - y

    def src_copy(s, c):
        return pltpu.make_async_copy(
            (saved_hbm, outcot_hbm)[s].at[pl.ds(c * chunk, chunk)],
            src.at[s, pl.ds(c * chunk, chunk)],
            src_sem.at[s, c],
        )

    def cot_copy(m):
        return pltpu.make_async_copy((qcot_hbm, fcot_hbm, mixed_hbm)[m], cot.at[m], cot_sem.at[m])

    def bas_copy(m):
        return pltpu.make_async_copy((qb_hbm, fb_hbm, ob_hbm)[m], bas.at[m], bas_sem.at[m])

    barrier = pltpu.get_barrier_semaphore()
    for k in range(1, n):
        pl.semaphore_signal(
            barrier, inc=1, device_id={"fs": lax.rem(me + k, n)}, device_id_type=MESH
        )
    for k in range(1, tp_n):
        pl.semaphore_signal(
            barrier, inc=1, device_id={"tp": lax.rem(tp + k, tp_n)}, device_id_type=MESH
        )

    bas_copy(0).start()
    src_copy(0, 0).start()
    cot_copy(0).start()
    for c in range(1, n_chunks):
        src_copy(0, c).start()
    bas_copy(1).start()
    cot_copy(1).start()
    bas_copy(2).start()
    for c in range(n_chunks):
        src_copy(1, c).start()
    cot_copy(2).start()

    for m in range(3):
        gath[m, me] = weights[m][...].astype(jnp.bfloat16)

    pl.semaphore_wait(barrier, n - 1 + tp_n - 1)

    def w_copy(m, block, target, send_sem):
        return pltpu.make_async_remote_copy(
            src_ref=gath.at[m, block],
            dst_ref=gath.at[m, block],
            send_sem=send_sem,
            recv_sem=w_recv.at[m, block],
            device_id={"fs": target},
            device_id_type=MESH,
        )

    def w_arrived(m, block):
        w_copy(m, block, partner, w_send.at[0, m, 0]).wait_recv()

    def w_round(r, act, wait, z=True, side=True):
        below, above = o - r, o + r
        for m in range(3):

            @pl.when(below >= 0)
            def _():
                block = below * 2 + y
                if wait and r > 0:
                    w_arrived(m, block)
                if z and r < half - 1:

                    @pl.when(o + 1 < half)
                    def _():
                        act(w_copy(m, block, me + 2, w_send.at[0, m, r]))

                if side:
                    act(w_copy(m, block, partner, w_send.at[2, m, r]))

            @pl.when(above < half)
            def _():
                block = above * 2 + y
                if wait and r > 0:
                    w_arrived(m, block)
                if z and r < half - 1:

                    @pl.when(o >= 1)
                    def _():
                        act(w_copy(m, block, me - 2, w_send.at[1, m, r]))

                if side and r > 0:
                    act(w_copy(m, block, partner, w_send.at[3, m, r]))

    def w_start(r, z=True, side=True):
        w_round(r, lambda copy: copy.start(), z, z, side)

    w_start(0)

    def rs_copy(m, k):
        peer = lax.rem(me + k, n)
        return pltpu.make_async_remote_copy(
            src_ref=part.at[m, pl.ds(pl.multiple_of(peer * rp, rp), rp)],
            dst_ref=rs_buf.at[m, k - 1],
            send_sem=rs_send.at[m, k - 1],
            recv_sem=rs_recv.at[m, k - 1],
            device_id={"fs": peer},
            device_id_type=MESH,
        )

    mine = pl.ds(pl.multiple_of(me * rp, rp), rp)

    def ag_copy(m, block, target, slot):
        at = pl.ds(pl.multiple_of(block * rp, rp), rp)
        return pltpu.make_async_remote_copy(
            src_ref=dirs.at[m, at],
            dst_ref=dirs.at[m, at],
            send_sem=ag_send.at[m, slot],
            recv_sem=ag_recv.at[m, block],
            device_id={"fs": target},
            device_id_type=MESH,
        )

    def ag_own(m):
        return [ag_copy(m, me, partner, 0)] + [
            ag_copy(m, me, lax.rem(o + d, half) * 2 + y, d) for d in range(1, half)
        ]

    def ag_forward(m):
        return [
            ag_copy(m, partner, lax.rem(o + d, half) * 2 + y, half - 1 + d)
            for d in range(1, half)
        ]

    def project(m):
        s = (0, 0, 1)[m]
        bas_copy(m).wait()
        cot_copy(m).wait()
        if m != 1:
            for c in range(n_chunks):
                src_copy(s, c).wait()

        acc[...] = jnp.zeros_like(acc)

        def body(c, carry):
            at = pl.ds(pl.multiple_of(c * chunk, chunk), chunk)
            reduced = jnp.dot(
                src[s, at, :], bas[m], preferred_element_type=jnp.float32
            ).astype(jnp.bfloat16)
            acc[...] += lax.dot_general(
                reduced,
                cot[m, at, :],
                (((0,), (0,)), ((), ())),
                preferred_element_type=jnp.float32,
            )
            return carry

        lax.fori_loop(0, n_chunks, body, 0)
        part[m] = acc[...].astype(jnp.bfloat16)
        for k in range(1, n):
            rs_copy(m, k).start()

    project(0)
    project(1)
    project(2)
    w_start(1)

    for m in range(3):
        projected = part[m, mine, :].astype(jnp.float32)
        for k in range(1, n):
            rs_copy(m, k).wait_recv()
            projected += rs_buf[m, k - 1].astype(jnp.float32)
        first_new = 0.8 * firsts[m][...] + 0.2 * projected
        second_new = 0.95 * seconds[m][...] + 0.05 * projected * projected
        firsts_new[m][...] = first_new
        seconds_new[m][...] = second_new
        direction = first_new / (jnp.sqrt(second_new) + 1e-08)
        dirs[m, mine, :] = direction.astype(jnp.bfloat16)
        for copy in ag_own(m):
            copy.start()

    for m in range(3):
        ag_copy(m, partner, partner, 0).wait_recv()
        for copy in ag_forward(m):
            copy.start()

    for r in range(2, half):
        w_start(r)

    sums = []
    for m in range(3):
        for d in range(1, half):
            for column in range(2):
                block = lax.rem(o + d, half) * 2 + column
                ag_copy(m, block, partner, 0).wait_recv()
        wide = dirs[m].astype(jnp.float32)
        sums.append(jnp.sum(wide * wide))
    line = lax.broadcasted_iota(jnp.int32, sq_own.shape, 0)
    sq_own[...] = jnp.where(line == 0, sums[0], jnp.where(line == 1, sums[1], sums[2]))

    def sq_copy(k):
        return pltpu.make_async_remote_copy(
            src_ref=sq_own,
            dst_ref=sq_buf.at[k - 1],
            send_sem=sq_send.at[k - 1],
            recv_sem=sq_recv.at[k - 1],
            device_id={"tp": lax.rem(tp + k, tp_n)},
            device_id_type=MESH,
        )

    for k in range(1, tp_n):
        sq_copy(k).start()
    total = sq_own[...]
    for k in range(1, tp_n):
        sq_copy(k).wait_recv()
        total += sq_buf[k - 1]
    scale = lax.rsqrt(total / (rank * cols * tp_n) + 1e-06)

    def out_copy(m, block):
        return pltpu.make_async_copy(
            stage.at[m, block],
            copies[m].at[pl.ds(pl.multiple_of(block * rows, rows), rows)],
            out_sem.at[m, block],
        )

    def step_of(m, block):
        at = pl.ds(pl.multiple_of(block * rows, rows), rows)
        return jnp.dot(bas[m, at, :], dirs[m], preferred_element_type=jnp.float32)

    for m in range(3):
        update = step_of(m, me) * scale[m : m + 1, :1]
        updates[m][...] = update
        stage[m, me] = (weights[m][...] - 0.05 * update).astype(jnp.bfloat16)
        out_copy(m, me).start()

    def finish(block, wait):
        for m in range(3):
            if wait:
                w_arrived(m, block)
            stage[m, block] = (
                gath[m, block].astype(jnp.float32)
                - step_of(m, block) * (0.05 * scale[m : m + 1, :1])
            ).astype(jnp.bfloat16)
            out_copy(m, block).start()

    def finish_at(distance, column, wait):
        @pl.when(o - distance >= 0)
        def _():
            finish((o - distance) * 2 + column, wait)

        if distance > 0:

            @pl.when(o + distance < half)
            def _():
                finish((o + distance) * 2 + column, wait)

    finish_at(0, 1 - y, True)
    for d in range(1, half):
        finish_at(d, y, False)
        finish_at(d, 1 - y, True)

    for r in range(half):
        w_round(r, lambda copy: copy.wait_send(), False)
    for m in range(3):
        for k in range(1, n):
            rs_copy(m, k).wait_send()
        for copy in ag_own(m) + ag_forward(m):
            copy.wait_send()
    for k in range(1, tp_n):
        sq_copy(k).wait_send()

    def drain(block, carry):
        for m in range(3):
            out_copy(m, block).wait()
        return carry

    lax.fori_loop(0, n, drain, 0)


def deliver(count, *refs):
    sources, targets, slots = refs[:count], refs[count : 2 * count], refs[2 * count : 3 * count]
    in_sem, out_sem = refs[3 * count :]

    def pieces(act_in, act_out):
        for i in range(count):
            rows = sources[i].shape[0]
            step = max(rows // 4, rows if rows <= 256 else 0)
            for p in range(rows // step):
                at = pl.ds(p * step, step)
                if act_in:
                    act_in(
                        pltpu.make_async_copy(
                            sources[i].at[at], slots[i].at[at], in_sem.at[i, p]
                        )
                    )
                if act_out:
                    act_out(
                        pltpu.make_async_copy(
                            slots[i].at[at], targets[i].at[at], out_sem.at[i, p]
                        )
                    )

    pieces(lambda copy: copy.start(), None)
    pieces(lambda copy: copy.wait(), lambda copy: copy.start())
    pieces(None, lambda copy: copy.wait())


def delivered(arrays):
    count = len(arrays)
    dma = pltpu.SemaphoreType.DMA
    return pl.pallas_call(
        functools.partial(deliver, count),
        out_shape=tuple(jax.ShapeDtypeStruct(a.shape, a.dtype) for a in arrays),
        in_specs=[pl.BlockSpec(memory_space=ANY)] * count,
        out_specs=(pl.BlockSpec(memory_space=ANY),) * count,
        scratch_shapes=[VMEM(a.shape, a.dtype) for a in arrays]
        + [dma((count, 4)), dma((count, 4))],
        compiler_params=pltpu.CompilerParams(vmem_limit_bytes=63 * 1024 * 1024),
    )(*arrays)


def local(
    n,
    tp_n,
    saved_input,
    query_cotangent,
    forget_cotangent,
    mixed_output,
    out_cotangent,
    query_basis,
    forget_basis,
    out_basis,
    query_weight,
    forget_weight,
    out_weight,
    query_first,
    forget_first,
    out_first,
    query_second,
    forget_second,
    out_second,
):
    tokens, width = saved_input.shape
    rank = query_basis.shape[1]
    rows, cols = query_weight.shape
    rp = rank // n
    half = n // 2
    chunk = min(512, tokens)
    f32, bf16 = jnp.float32, jnp.bfloat16
    dma = pltpu.SemaphoreType.DMA
    shape = jax.ShapeDtypeStruct
    results = pl.pallas_call(
        functools.partial(kernel, n, tp_n, chunk),
        out_shape=(shape((rows, cols), f32),) * 3
        + (shape((rp, cols), f32),) * 6
        + (shape((n * rows, cols), bf16),) * 3,
        in_specs=[pl.BlockSpec(memory_space=ANY)] * 8 + [pl.BlockSpec(memory_space=VMEM)] * 9,
        out_specs=(pl.BlockSpec(memory_space=VMEM),) * 9 + (pl.BlockSpec(memory_space=ANY),) * 3,
        scratch_shapes=[
            VMEM((2, tokens, width), bf16),
            VMEM((3, tokens, cols), bf16),
            VMEM((3, width, rank), bf16),
            VMEM((rank, cols), f32),
            VMEM((3, rank, cols), bf16),
            VMEM((3, n - 1, rp, cols), bf16),
            VMEM((3, rank, cols), bf16),
            VMEM((3, n, rows, cols), bf16),
            VMEM((3, n, rows, cols), bf16),
            VMEM((8, 128), f32),
            VMEM((tp_n - 1, 8, 128), f32),
            dma((2, tokens // chunk)),
            dma((3,)),
            dma((3,)),
            dma((3, n - 1)),
            dma((3, n - 1)),
            dma((3, n - 1)),
            dma((3, n)),
            dma((4, 3, half)),
            dma((3, n)),
            dma((tp_n - 1,)),
            dma((tp_n - 1,)),
            dma((3, n)),
        ],
        compiler_params=pltpu.CompilerParams(
            collective_id=0, has_side_effects=True, vmem_limit_bytes=63 * 1024 * 1024
        ),
    )(
        saved_input,
        out_cotangent,
        query_cotangent,
        forget_cotangent,
        mixed_output,
        query_basis,
        forget_basis,
        out_basis,
        query_weight,
        forget_weight,
        out_weight,
        query_first,
        forget_first,
        out_first,
        query_second,
        forget_second,
        out_second,
    )
    return delivered(results)


def solution(mesh):
    split = P("fs", "tp")
    in_specs = (
        (P("fs", None), split, split, split, P("fs", None)) + (P(),) * 3 + (split,) * 9
    )
    out_specs = (split,) * 9 + (P(None, "tp"),) * 3
    return jax.shard_map(
        functools.partial(local, mesh.shape["fs"], mesh.shape["tp"]),
        mesh=mesh,
        in_specs=in_specs,
        out_specs=out_specs,
        check_vma=False,
    )
```
